32 devices in a mesh: ep: 8 (over z, y), tp: 4 (over x, core).
Axes of the slice: x: 2, y: 2, z: 4, core: 2. Of those that a mesh axis runs over, the one named last changes fastest.
Arguments:
- queries: bfloat16 [8192, 1024], P('ep', 'tp'), may hold values from -6 to 6
- head_keys: bfloat16 [8192, 256], P('ep', 'tp'), may hold values from -6 to 6
- head_values: bfloat16 [8192, 256], P('ep', 'tp'), may hold values from -6 to 6
- sink_logits: float32 [16], P('tp'), may hold values from -2 to 5
- out_weight: bfloat16 [1024, 2048], P('tp'), may hold values from -1.5 to 1.5
- moe_input: bfloat16 [4096, 2048], P(('ep', 'tp')), may hold values from -6 to 6
- norm_gain: float32 [2048], replicated, may hold values from 0.1 to 1.9
- routes: int32 [4096, 4], P(('ep', 'tp')), may hold values from 0 to 7, all different within a row; in each aligned block of 128 rows (0 to 127, 128 to 255, ...) at most 128 rows name the same one
- route_weight: float32 [4096, 4], P(('ep', 'tp')), may hold values from 0.05 to 1
- gate_weight: bfloat16 [8, 2048, 512], P('ep'), may hold values from -2 to 2
- up_weight: bfloat16 [8, 2048, 512], P('ep'), may hold values from -2 to 2
- down_weight: bfloat16 [8, 512, 2048], P('ep'), may hold values from -0.25 to 0.25
Outputs:
- attention_out: bfloat16 [8192, 2048], P(('ep', 'tp'))
- routed_out: bfloat16 [4096, 2048], P(('ep', 'tp'))
The draws below stay inside these ranges and needn't reach their ends.
Inputs may be any that keep to these rules, and one draw needn't show every extreme that they name: `routes`: within the rows of one device (aligned blocks of 128 rows), each expert is named by at most 128 rows, and in every draw some expert by exactly 128; a row names 4 different experts.
All inputs are finite; a program needn't handle non-finite values.
Results may differ from the reference program's by a relative error of at most 0.0078.
Values may be sent and summed in bfloat16 or wider, within the bound.
No kernel may reach another device: no remote copies, remote signals or barrier semaphores. Data moves between devices by JAX's collectives and lax.ppermute only.
A program may use at most 128 MiB of HBM per device.

```python
import math
import jax
import jax.numpy as jnp
import numpy as np
from jax import lax

D = 2048
HEADS = 16
KV_HEADS = 4
HEAD_DIM = 64
WINDOW = 128
SEQS = 1
FF = 512
TOPK = 4
TOK_M = 128
EXPERTS = 8
CAP = 128
TOKENS_A = 8192
TOKENS_M = 4096


def draw_queries(key, part):
    per_group = HEADS // KV_HEADS
    normal = jax.random.normal(jax.random.fold_in(key, 1), (TOKENS_A, KV_HEADS, per_group, HEAD_DIM), jnp.float32)
    normal = jnp.clip(normal, -6.0, 6.0)
    return normal.reshape(TOKENS_A, HEADS * HEAD_DIM).astype(jnp.bfloat16)


def draw_head_keys(key, part):
    normal = jax.random.normal(jax.random.fold_in(key, 2), (TOKENS_A, KV_HEADS, 1, HEAD_DIM), jnp.float32)
    normal = jnp.clip(normal, -6.0, 6.0)
    return normal.reshape(TOKENS_A, KV_HEADS * HEAD_DIM).astype(jnp.bfloat16)


def expert_matrix(key, salt):
    normal = jax.random.normal(jax.random.fold_in(key, salt), (EXPERTS, D, FF), jnp.float32)
    normal = jnp.clip(normal, -6.0, 6.0) * D ** (-0.5)
    return jnp.clip(normal, -2.0, 2.0).astype(jnp.bfloat16)


def draw_gate_weight(key, part):
    return expert_matrix(key, 11)


def draw_up_weight(key, part):
    return expert_matrix(key, 13)


def block_scale(stream_key, shape, pieces, low, top_value):
    factor_of, own = 1.0, jax.random.fold_in(stream_key, 6)
    for position, parts in pieces:
        draws = jnp.exp(jax.random.uniform(jax.random.fold_in(own, position), (parts,), jnp.float32, low / len(pieces), top_value / len(pieces)))
        factor_of = factor_of * jnp.repeat(draws, shape[position] // parts).reshape([-1 if axis == position else 1 for axis in range(len(shape))])
    return factor_of


def deal_out(key, own, number, rows, number_of, top, limit, lean):
    sequence = jax.random.permutation(key, number_of)
    crowded, ordinary = shares(number_of, rows * top, limit, lean, True), shares(number_of, rows * top, limit, lean, False)
    places = jnp.arange(number_of)

    def named(tallies, turn):
        used = int((tallies > 0).sum())
        fixed = max(1, used // 4)
        passed = fixed + (places - fixed + turn * (used - fixed)) % max(1, number_of - fixed)
        return jnp.zeros((number_of,), jnp.int32).at[sequence[jnp.where(places < fixed, places, passed)]].set(jnp.asarray(tallies, jnp.int32))

    tallies = jnp.where(number % 4 == 0, named(crowded, number // 4), named(ordinary, number - number // 4 - 1))
    mixed = jax.random.permutation(jax.random.fold_in(own, 3), number_of)
    giver, sink = mixed[0:number_of // 2 * 2:2], mixed[1:number_of // 2 * 2:2]
    margin = jnp.minimum(tallies[giver] - 1, limit - tallies[sink]) // 2
    margin = jnp.where((giver == sequence[0]) | (sink == sequence[0]) | (tallies[sink] == 0), 0, jnp.maximum(margin, 0))
    passed = jax.random.randint(jax.random.fold_in(own, 4), (number_of // 2,), 0, 1 << 20) % (margin + 1)
    tallies = tallies.at[giver].add(-passed).at[sink].add(passed)
    labels = jnp.searchsorted(jnp.cumsum(tallies), jnp.arange(rows * top), side="right").astype(jnp.int32)
    listing = labels.reshape(top, rows).T
    listing = listing[jax.random.permutation(jax.random.fold_in(own, 1), rows)]
    turn = jax.random.randint(jax.random.fold_in(own, 2), (rows, 1), 0, top)
    return jnp.take_along_axis(listing, (jnp.arange(top)[None, :] + turn) % top, axis=1)


def shares(number_of, total, most, skew, full):
    portions = [(1 << 20) // math.isqrt(standing ** skew) + 1 for standing in range(1, number_of + 1)]
    largest = most if full else min(most, max(-(-total // number_of), total * portions[0] // sum(portions)))
    least = 1 if total - largest >= number_of - 1 else 0
    given, rest = [largest] + [least] * (number_of - 1), total - largest - least * (number_of - 1)
    while rest > 0:
        candidates = [i for i in range(1, number_of) if given[i] < largest] or [i for i in range(1, number_of) if given[i] < most]
        mass, remaining = sum([portions[i] for i in candidates]), rest
        for i in candidates:
            addition = min(most - given[i], max(1, remaining * portions[i] // mass), rest)
            given[i] = given[i] + addition
            rest = rest - addition
    return np.array(given)


def gaussian(key, shape, spread, reach, split=(), kind=jnp.bfloat16):
    drawn = jax.random.normal(key, shape, jnp.float32) * spread
    if len(split) > 0:
        drawn = block_scale(key, shape, split, -0.22, 0.18) * drawn
    return jnp.clip(drawn, min=-reach, max=reach).astype(kind)


def setup_inputs(seed: int = 0) -> dict:
    streams_of = jax.random.split(jax.random.key(seed), 13)
    queries = draw_queries(jax.random.fold_in(streams_of[12], 71), 0)
    head_keys = draw_head_keys(jax.random.fold_in(streams_of[12], 71), 0)
    head_values = gaussian(streams_of[2], (TOKENS_A, KV_HEADS * HEAD_DIM), 1.0, 6.0, ((0, 8), (1, 4)))
    sink_logits = jnp.clip(-2.0 + 7.0 * jax.random.uniform(streams_of[3], (HEADS,), jnp.float32) ** block_scale(streams_of[3], (HEADS,), ((0, 4),), -0.2, 0.2), -2.0, 5.0)
    out_weight = gaussian(streams_of[4], (HEADS * HEAD_DIM, D), 0.25, 1.5, ((0, 4),))
    moe_input = gaussian(streams_of[5], (TOKENS_M, D), 1.0, 6.0, ((0, 32),))
    norm_gain = jnp.clip(1.0 + 0.18 * jax.random.normal(streams_of[6], (D,), jnp.float32), 0.1, 1.9)
    routes_keys = jax.random.split(jax.random.fold_in(streams_of[7], 1), TOKENS_M // TOK_M)
    routes_turns = jax.random.permutation(jax.random.fold_in(streams_of[7], 3), TOKENS_M // TOK_M)
    routes = jax.vmap(lambda own, number: deal_out(jax.random.fold_in(streams_of[7], 2), own, number, TOK_M, EXPERTS, TOPK, CAP, 1))(routes_keys, routes_turns).reshape((TOKENS_M, TOPK))
    route_weight = jnp.clip(jnp.exp(math.log(1.0) - 2.9957323 * jax.random.uniform(streams_of[8], (TOKENS_M, TOPK), jnp.float32) ** block_scale(streams_of[8], (TOKENS_M, TOPK), ((0, 32),), -0.2, 0.2)), 0.05, 1.0)
    gate_weight = draw_gate_weight(jax.random.fold_in(streams_of[12], 71), 0)
    up_weight = draw_up_weight(jax.random.fold_in(streams_of[12], 71), 0)
    down_weight = gaussian(streams_of[11], (EXPERTS, FF, D), FF ** -0.5, 0.25, ((0, 8),))
    return dict(queries=queries, head_keys=head_keys, head_values=head_values, sink_logits=sink_logits, out_weight=out_weight, moe_input=moe_input, norm_gain=norm_gain, routes=routes, route_weight=route_weight, gate_weight=gate_weight, up_weight=up_weight, down_weight=down_weight)


EPSILON = 1e-05
NEGATIVE = -1e+30

def clamped_unit(gate_pre, up_pre):
    gate_cut = jnp.minimum(gate_pre, 7.0)
    up_cut = jnp.clip(up_pre, -7.0, 7.0)
    return gate_cut * jax.nn.sigmoid(1.702 * gate_cut) * (up_cut + 1.0)

def window_attention(queries, head_keys, head_values, sink_logits, out_weight):
    total = queries.shape[0]
    per_group = HEADS // KV_HEADS
    seq_len = TOKENS_A // SEQS
    padding = jnp.zeros((WINDOW, KV_HEADS * HEAD_DIM), head_keys.dtype)
    padded_keys = jnp.concatenate([padding, head_keys], axis=0)
    padded_values = jnp.concatenate([padding, head_values], axis=0)
    sinks = sink_logits.astype(jnp.float32).reshape(KV_HEADS, per_group, 1, 1)

    def one_block(index):
        first = (index * WINDOW).astype(jnp.int32)
        block_q = lax.dynamic_slice_in_dim(queries, first, WINDOW, 0)
        block_q = block_q.reshape(WINDOW, KV_HEADS, per_group, HEAD_DIM).astype(jnp.float32)
        block_k = lax.dynamic_slice_in_dim(padded_keys, first, 2 * WINDOW, 0)
        block_k = block_k.reshape(2 * WINDOW, KV_HEADS, HEAD_DIM).astype(jnp.float32)
        block_v = lax.dynamic_slice_in_dim(padded_values, first, 2 * WINDOW, 0)
        block_v = block_v.reshape(2 * WINDOW, KV_HEADS, HEAD_DIM).astype(jnp.float32)
        scores = jnp.einsum('qkgd,skd->kgqs', block_q, block_k) * HEAD_DIM ** (-0.5)
        query_pos = first + jnp.arange(WINDOW, dtype=jnp.int32)
        key_pos = first - WINDOW + jnp.arange(2 * WINDOW, dtype=jnp.int32)
        distance = query_pos[:, None] - key_pos[None, :]
        starts = query_pos // seq_len * seq_len
        valid = (distance >= 0) & (distance < WINDOW) & (key_pos[None, :] >= starts[:, None])
        scores = jnp.where(valid[None, None], scores, NEGATIVE)
        maxima = jnp.maximum(lax.optimization_barrier(jnp.max(scores, axis=-1, keepdims=True)), sinks)
        powers = jnp.exp(scores - maxima)
        weights = powers / (lax.optimization_barrier(jnp.sum(powers, axis=-1, keepdims=True)) + jnp.exp(sinks - maxima))
        weights = weights.astype(jnp.bfloat16)
        heads = jnp.einsum('kgqs,skd->qkgd', weights.astype(jnp.float32), block_v)
        return heads.astype(jnp.bfloat16).reshape(WINDOW, HEADS * HEAD_DIM)
    heads_out = lax.map(one_block, jnp.arange(total // WINDOW, dtype=jnp.int32))
    heads_out = heads_out.reshape(total, HEADS * HEAD_DIM)
    return jnp.dot(heads_out, out_weight, preferred_element_type=jnp.float32).astype(jnp.bfloat16)

def routed_experts(moe_input, norm_gain, routes, route_weight, gate_weight, up_weight, down_weight):
    token_count = moe_input.shape[0]
    values32 = moe_input.astype(jnp.float32)
    scale = lax.rsqrt(lax.optimization_barrier(jnp.mean(values32 * values32, axis=-1, keepdims=True)) + EPSILON)
    normed = (values32 * scale * norm_gain.astype(jnp.float32)).astype(jnp.bfloat16)
    assigned = token_count * TOPK
    group_rows = 256
    flat_routes = routes.reshape(assigned).astype(jnp.int32)
    token_of = (jnp.arange(assigned, dtype=jnp.int32) // TOPK).astype(jnp.int32)
    order = jnp.argsort(flat_routes, stable=True).astype(jnp.int32)
    sorted_routes = flat_routes[order]
    counts = lax.optimization_barrier(jnp.sum((flat_routes[:, None] == jnp.arange(EXPERTS, dtype=jnp.int32)[None, :]).astype(jnp.int32), axis=0)).astype(jnp.int32)
    padded = ((counts + group_rows - 1) // group_rows * group_rows).astype(jnp.int32)
    end_pad = jnp.cumsum(padded).astype(jnp.int32)
    start_pad = (end_pad - padded).astype(jnp.int32)
    start_raw = (jnp.cumsum(counts) - counts).astype(jnp.int32)
    dest = (start_pad[sorted_routes] + jnp.arange(assigned, dtype=jnp.int32) - start_raw[sorted_routes]).astype(jnp.int32)
    group_count = -(-assigned // group_rows) + EXPERTS
    slot_total = group_count * group_rows
    row_token = jnp.zeros((slot_total,), jnp.int32).at[dest].set(token_of[order])
    row_weight = jnp.zeros((slot_total,), jnp.float32).at[dest].set(route_weight.reshape(assigned).astype(jnp.float32)[order])
    group_expert = jnp.searchsorted(end_pad, jnp.arange(group_count, dtype=jnp.int32) * group_rows, side='right')
    group_expert = jnp.minimum(group_expert, EXPERTS - 1).astype(jnp.int32)

    def add_group(total, inputs):
        expert, tokens, weights = inputs
        rows_in = normed[tokens]
        gate_pre = jnp.dot(rows_in, gate_weight[expert], preferred_element_type=jnp.float32)
        up_pre = jnp.dot(rows_in, up_weight[expert], preferred_element_type=jnp.float32)
        act = clamped_unit(gate_pre, up_pre).astype(jnp.bfloat16)
        result = jnp.dot(act, down_weight[expert], preferred_element_type=jnp.float32).astype(jnp.bfloat16)
        return (total.at[tokens].add(result.astype(jnp.float32) * weights[:, None]), None)
    initial = jnp.zeros((token_count, D), jnp.float32)
    total, _ = lax.scan(add_group, initial, (group_expert, row_token.reshape(group_count, group_rows), row_weight.reshape(group_count, group_rows)))
    return total.astype(jnp.bfloat16)

def reference(queries, head_keys, head_values, sink_logits, out_weight, moe_input, norm_gain, routes, route_weight, gate_weight, up_weight, down_weight):
    attention_out = window_attention(queries, head_keys, head_values, sink_logits, out_weight)
    routed_out = routed_experts(moe_input, norm_gain, routes, route_weight, gate_weight, up_weight, down_weight)
    return (attention_out, routed_out)
```

```python
import jax
import jax.numpy as jnp
from jax import lax
from jax.sharding import PartitionSpec as P

HEAD_DIM = 64
WINDOW = 128
SEQS = 1


EPSILON = 1e-05
NEGATIVE = -1e30
LANES = 128


def passed_along(value, axis, steps):
    count = lax.axis_size(axis)
    first, last = (max(0, -steps), min(count, count - steps))
    return lax.ppermute(value, axis, [(source, source + steps) for source in range(first, last)])


def clamped_unit(gate_pre, up_pre):
    gate_cut = jnp.minimum(gate_pre, 7.0)
    up_cut = jnp.clip(up_pre, -7.0, 7.0)
    return gate_cut * jax.nn.sigmoid(1.702 * gate_cut) * (up_cut + 1.0)


def attend(queries, head_keys, head_values, sink_logits, out_weight):
    tok_rows = queries.shape[0]
    local_heads = sink_logits.shape[0]
    local_kv = head_keys.shape[1] // HEAD_DIM
    per_group = local_heads // local_kv
    block_count = tok_rows // WINDOW
    key_width = local_kv * HEAD_DIM
    kv_rows = jnp.concatenate([head_keys, head_values], axis=1)
    earlier = passed_along(kv_rows[tok_rows - WINDOW :], "ep", 1)
    extended = jnp.concatenate([earlier, kv_rows], axis=0)
    banded = jnp.concatenate(
        [
            extended[:tok_rows].reshape(block_count, WINDOW, 2 * key_width),
            kv_rows.reshape(block_count, WINDOW, 2 * key_width),
        ],
        axis=1,
    )
    band_keys = banded[:, :, :key_width].reshape(block_count, 2 * WINDOW, local_kv, HEAD_DIM)
    band_values = banded[:, :, key_width:].reshape(block_count, 2 * WINDOW, local_kv, HEAD_DIM)
    blocked = queries.reshape(block_count, WINDOW, local_kv, per_group, HEAD_DIM)
    scores = jnp.einsum(
        "nqkgd,nskd->nkgqs", blocked, band_keys, preferred_element_type=jnp.float32
    ) * HEAD_DIM ** (-0.5)
    offset = lax.axis_index("ep") * tok_rows
    seq_len = tok_rows * lax.axis_size("ep") // SEQS
    query_pos = offset + jnp.arange(tok_rows, dtype=jnp.int32).reshape(block_count, WINDOW)
    key_pos = (
        offset
        - WINDOW
        + (jnp.arange(block_count, dtype=jnp.int32) * WINDOW)[:, None]
        + jnp.arange(2 * WINDOW, dtype=jnp.int32)[None, :]
    )
    distance = query_pos[:, :, None] - key_pos[:, None, :]
    starts = query_pos // seq_len * seq_len
    valid = (distance >= 0) & (distance < WINDOW) & (key_pos[:, None, :] >= starts[:, :, None])
    scores = jnp.where(valid[:, None, None], scores, NEGATIVE)
    sinks = sink_logits.reshape(local_kv, per_group, 1, 1)
    maxima = jnp.maximum(jnp.max(scores, axis=-1, keepdims=True), sinks)
    powers = jnp.exp(scores - maxima)
    weights = (powers / (jnp.sum(powers, axis=-1, keepdims=True) + jnp.exp(sinks - maxima))).astype(
        jnp.bfloat16
    )
    heads_out = jnp.einsum(
        "nkgqs,nskd->nqkgd", weights, band_values, preferred_element_type=jnp.float32
    )
    heads_out = heads_out.astype(jnp.bfloat16).reshape(tok_rows, local_heads * HEAD_DIM)
    return project(heads_out, out_weight)


def swapped(value, axis, pattern):
    count = lax.axis_size(axis)
    return lax.ppermute(value, axis, [(source, source ^ pattern) for source in range(count)])


def gathered_weights(out_weight):
    count = lax.axis_size("tp")
    pieces = {0: out_weight}
    step = count // 2
    while step:
        for pattern in sorted(pieces):
            pieces[pattern ^ step] = swapped(pieces[pattern], "tp", step)
        step //= 2
    return pieces


def project(heads_out, out_weight):
    count = lax.axis_size("tp")
    rows = heads_out.shape[0] // count
    mine = lax.axis_index("tp")
    weights = gathered_weights(out_weight)
    total = None
    for pattern in range(count):
        part = lax.dynamic_slice_in_dim(heads_out, (mine ^ pattern) * rows, rows, 0)
        if pattern:
            part = swapped(part, "tp", pattern)
        product = jnp.dot(part, weights[pattern], preferred_element_type=jnp.float32)
        total = product if total is None else total + product
    return total.astype(jnp.bfloat16)


def experts_part(moe_input, norm_gain, routes, route_weight, gate_weight, up_weight, down_weight):
    tok_rows, model_width = moe_input.shape
    choice_count = routes.shape[1]
    targets = lax.axis_size("ep")
    capacity = 2 * choice_count * tok_rows // targets
    values32 = moe_input.astype(jnp.float32)
    scale = lax.rsqrt(jnp.mean(values32 * values32, axis=-1, keepdims=True) + EPSILON)
    normed = (values32 * scale * norm_gain).astype(jnp.bfloat16)
    flat_routes = routes.reshape(-1)
    onehot = (flat_routes[:, None] == jnp.arange(targets, dtype=jnp.int32)[None, :]).astype(
        jnp.int32
    )
    earlier_count = jnp.sum((jnp.cumsum(onehot, axis=0) - onehot) * onehot, axis=1)
    slot_index = flat_routes * capacity + earlier_count
    copies = jnp.repeat(normed, choice_count, axis=0)
    outgoing = jnp.zeros((targets * capacity, model_width), jnp.bfloat16).at[slot_index].set(copies)
    outgoing = outgoing.reshape(targets, capacity, model_width)
    arrived = lax.all_to_all(outgoing, "ep", split_axis=0, concat_axis=0, tiled=True)
    flat_rows = arrived.reshape(-1, model_width)
    gate_pre = jnp.dot(flat_rows, gate_weight[0], preferred_element_type=jnp.float32)
    up_pre = jnp.dot(flat_rows, up_weight[0], preferred_element_type=jnp.float32)
    act = clamped_unit(gate_pre, up_pre).astype(jnp.bfloat16)
    result = jnp.dot(act, down_weight[0], preferred_element_type=jnp.float32).astype(jnp.bfloat16)
    came_back = lax.all_to_all(
        result.reshape(arrived.shape), "ep", split_axis=0, concat_axis=0, tiled=True
    )
    picked = came_back.reshape(targets * capacity, model_width)[slot_index]
    weighted = (
        picked.astype(jnp.float32).reshape(tok_rows, choice_count, model_width)
        * route_weight[:, :, None]
    )
    return jnp.sum(weighted, axis=1).astype(jnp.bfloat16)


def ring_pairs(count, step):
    order = list(range(0, count, 2)) + list(range(count - 1, 0, -2))
    return [(order[at], order[(at + step) % count]) for at in range(count)]


def onward(value):
    return lax.ppermute(value, "ep", ring_pairs(lax.axis_size("ep"), 1))


def backward(value):
    return lax.ppermute(value, "ep", ring_pairs(lax.axis_size("ep"), -1))


def ring_experts(moe_input, norm_gain, routes, route_weight, gate_weight, up_weight, down_weight):
    tok_rows, model_width = moe_input.shape
    targets = lax.axis_size("ep")
    half = targets // 2
    cut = tok_rows // 2
    mine = lax.axis_index("ep")
    values32 = moe_input.astype(jnp.float32)
    scale = lax.rsqrt(jnp.mean(values32 * values32, axis=-1, keepdims=True) + EPSILON)
    normed = (values32 * scale * norm_gain).astype(jnp.bfloat16)
    chosen = routes[:, :, None] == jnp.arange(LANES // 2, dtype=jnp.int32)[None, None, :]
    shares = jnp.sum(jnp.where(chosen, route_weight[:, :, None], 0.0), axis=1)
    coarse = lax.reduce_precision(shares, 8, 7)
    columns = jnp.concatenate([coarse, shares - coarse], axis=1).astype(jnp.bfloat16)
    block = jnp.concatenate([normed, columns], axis=1)
    lane = jnp.arange(LANES, dtype=jnp.int32) % (LANES // 2)

    def expert(rows):
        features = rows[:, :model_width]
        weight = jnp.sum(
            jnp.where(lane == mine, rows[:, model_width:].astype(jnp.float32), 0.0),
            axis=1,
            keepdims=True,
        )
        gate_pre = jnp.dot(features, gate_weight[0], preferred_element_type=jnp.float32)
        up_pre = jnp.dot(features, up_weight[0], preferred_element_type=jnp.float32)
        act = clamped_unit(gate_pre, up_pre).astype(jnp.bfloat16)
        result = jnp.dot(act, down_weight[0], preferred_element_type=jnp.float32)
        return result.astype(jnp.bfloat16), weight

    def share(pair, start, stop):
        return pair[0][start:stop].astype(jnp.float32) * pair[1][start:stop]

    results = {}
    ahead = behind = block
    for step in range(1, half):
        ahead, behind = onward(ahead), backward(behind)
        if step == 1:
            both = expert(jnp.concatenate([block, ahead, behind], axis=0))
            results[0] = share(both, 0, tok_rows)
            results[-1] = share(both, tok_rows, 2 * tok_rows)
            results[1] = share(both, 2 * tok_rows, 3 * tok_rows)
        else:
            both = expert(jnp.concatenate([ahead, behind], axis=0))
            results[-step] = share(both, 0, tok_rows)
            results[step] = share(both, tok_rows, 2 * tok_rows)
    far_ahead, far_behind = onward(ahead[:cut]), backward(behind[cut:])
    far = expert(jnp.concatenate([far_ahead, far_behind], axis=0))
    first, second = onward(share(far, 0, cut).astype(jnp.bfloat16)), backward(
        share(far, cut, tok_rows).astype(jnp.bfloat16)
    )
    up_sum = jnp.concatenate(
        [results[half - 1][:cut] + first.astype(jnp.float32), results[half - 1][cut:]], axis=0
    )
    down_sum = jnp.concatenate(
        [results[1 - half][:cut], results[1 - half][cut:] + second.astype(jnp.float32)], axis=0
    )
    for step in range(half - 1, 0, -1):
        up_sum = onward(up_sum.astype(jnp.bfloat16)).astype(jnp.float32)
        down_sum = backward(down_sum.astype(jnp.bfloat16)).astype(jnp.float32)
        if step > 1:
            up_sum = up_sum + results[step - 1]
            down_sum = down_sum + results[1 - step]
    return (results[0] + up_sum + down_sum).astype(jnp.bfloat16)


def on_device(
    queries,
    head_keys,
    head_values,
    sink_logits,
    out_weight,
    moe_input,
    norm_gain,
    routes,
    route_weight,
    gate_weight,
    up_weight,
    down_weight,
):
    attention_out = attend(queries, head_keys, head_values, sink_logits, out_weight)
    targets = lax.axis_size("ep")
    dense = targets % 2 == 0 and 4 <= targets <= 4 * routes.shape[1]
    routed_out = (ring_experts if dense else experts_part)(
        moe_input, norm_gain, routes, route_weight, gate_weight, up_weight, down_weight
    )
    return (attention_out, routed_out)


def solution(mesh):
    placed = (
        P("ep", "tp"),
        P("ep", "tp"),
        P("ep", "tp"),
        P("tp"),
        P("tp", None),
        P(("ep", "tp"), None),
        P(),
        P(("ep", "tp"), None),
        P(("ep", "tp"), None),
        P("ep", None, None),
        P("ep", None, None),
        P("ep", None, None),
    )
    return jax.shard_map(
        on_device,
        mesh=mesh,
        in_specs=placed,
        out_specs=(P(("ep", "tp"), None), P(("ep", "tp"), None)),
        check_vma=False,
    )
```

```python
import functools

import jax
import jax.numpy as jnp
from jax import lax
from jax.experimental import pallas as pl
from jax.experimental.pallas import tpu as pltpu
from jax.sharding import PartitionSpec as P


HEAD_DIM = 64
WINDOW = 128
SEQS = 1


EPSILON = 1e-05
NEGATIVE = -1e30


def passed_along(value, axis, steps):
    count = lax.axis_size(axis)
    first, last = (max(0, -steps), min(count, count - steps))
    return lax.ppermute(value, axis, [(source, source + steps) for source in range(first, last)])


def clamped_unit(gate_pre, up_pre):
    gate_cut = jnp.minimum(gate_pre, 7.0)
    up_cut = jnp.clip(up_pre, -7.0, 7.0)
    return gate_cut * jax.nn.sigmoid(1.702 * gate_cut) * (up_cut + 1.0)


def band_kernel(
    offset_ref,
    sinks_ref,
    queries_ref,
    keys_ref,
    keys_before_ref,
    values_ref,
    values_before_ref,
    earlier_ref,
    out_ref,
    *,
    seq_len,
    per_group,
    key_width,
):
    block = pl.program_id(0)
    position = offset_ref[0] + block * WINDOW
    keys_before = jnp.where(block == 0, earlier_ref[:, :key_width], keys_before_ref[...])
    values_before = jnp.where(block == 0, earlier_ref[:, key_width:], values_before_ref[...])
    shape = (WINDOW, 2 * WINDOW)
    place = lax.broadcasted_iota(jnp.int32, shape, 1)
    distance = lax.broadcasted_iota(jnp.int32, shape, 0) + WINDOW - place
    least = jnp.where(lax.rem(position, seq_len) == 0, WINDOW, 0)
    valid = (distance >= 0) & (distance < WINDOW) & (place >= least)
    for group in range(key_width // HEAD_DIM):
        at = slice(group * HEAD_DIM, (group + 1) * HEAD_DIM)
        keys = jnp.concatenate([keys_before[:, at], keys_ref[:, at]], axis=0)
        values = jnp.concatenate([values_before[:, at], values_ref[:, at]], axis=0)
        for head in range(group * per_group, (group + 1) * per_group):
            columns = slice(head * HEAD_DIM, (head + 1) * HEAD_DIM)
            scores = lax.dot_general(
                queries_ref[:, columns],
                keys,
                (((1,), (1,)), ((), ())),
                preferred_element_type=jnp.float32,
            ) * HEAD_DIM ** (-0.5)
            scores = jnp.where(valid, scores, NEGATIVE)
            sink = sinks_ref[head]
            maxima = jnp.maximum(jnp.max(scores, axis=-1, keepdims=True), sink)
            powers = jnp.exp(scores - maxima)
            total = jnp.sum(powers, axis=-1, keepdims=True) + jnp.exp(sink - maxima)
            weights = (powers / total).astype(jnp.bfloat16)
            out_ref[:, columns] = jnp.dot(
                weights, values, preferred_element_type=jnp.float32
            ).astype(jnp.bfloat16)


def attend(queries, head_keys, head_values, sink_logits, out_weight):
    tok_rows = queries.shape[0]
    local_heads = sink_logits.shape[0]
    local_kv = head_keys.shape[1] // HEAD_DIM
    per_group = local_heads // local_kv
    key_width = local_kv * HEAD_DIM
    width = local_heads * HEAD_DIM
    tail = jnp.concatenate(
        [head_keys[tok_rows - WINDOW :], head_values[tok_rows - WINDOW :]], axis=1
    )
    earlier = passed_along(tail, "ep", 1)
    offset = (lax.axis_index("ep") * tok_rows).astype(jnp.int32).reshape(1)
    seq_len = tok_rows * lax.axis_size("ep") // SEQS
    heads_out = pl.pallas_call(
        functools.partial(band_kernel, seq_len=seq_len, per_group=per_group, key_width=key_width),
        grid=(tok_rows // WINDOW,),
        in_specs=[
            pl.BlockSpec(memory_space=pltpu.SMEM),
            pl.BlockSpec(memory_space=pltpu.SMEM),
            pl.BlockSpec((WINDOW, width), lambda n: (n, 0)),
            pl.BlockSpec((WINDOW, key_width), lambda n: (n, 0)),
            pl.BlockSpec((WINDOW, key_width), lambda n: (jnp.maximum(n - 1, 0), 0)),
            pl.BlockSpec((WINDOW, key_width), lambda n: (n, 0)),
            pl.BlockSpec((WINDOW, key_width), lambda n: (jnp.maximum(n - 1, 0), 0)),
            pl.BlockSpec((WINDOW, 2 * key_width), lambda n: (0, 0)),
        ],
        out_specs=pl.BlockSpec((WINDOW, width), lambda n: (n, 0)),
        out_shape=jax.ShapeDtypeStruct((tok_rows, width), jnp.bfloat16),
        name="band_attention",
    )(
        offset,
        sink_logits,
        queries,
        head_keys,
        head_keys,
        head_values,
        head_values,
        earlier,
    )
    return project(heads_out, out_weight)


def swapped(value, axis, pattern):
    count = lax.axis_size(axis)
    return lax.ppermute(value, axis, [(source, source ^ pattern) for source in range(count)])


def gathered_weights(out_weight):
    count = lax.axis_size("tp")
    pieces = {0: out_weight}
    step = count // 2
    while step:
        for pattern in sorted(pieces):
            pieces[pattern ^ step] = swapped(pieces[pattern], "tp", step)
        step //= 2
    return pieces


def project(heads_out, out_weight):
    count = lax.axis_size("tp")
    rows = heads_out.shape[0] // count
    mine = lax.axis_index("tp")
    weights = gathered_weights(out_weight)
    total = None
    for pattern in range(count):
        part = lax.dynamic_slice_in_dim(heads_out, (mine ^ pattern) * rows, rows, 0)
        if pattern:
            part = swapped(part, "tp", pattern)
        product = jnp.dot(part, weights[pattern], preferred_element_type=jnp.float32)
        total = product if total is None else total + product
    return total.astype(jnp.bfloat16)


def experts_part(moe_input, norm_gain, routes, route_weight, gate_weight, up_weight, down_weight):
    tok_rows, model_width = moe_input.shape
    choice_count = routes.shape[1]
    targets = lax.axis_size("ep")
    capacity = 2 * choice_count * tok_rows // targets
    values32 = moe_input.astype(jnp.float32)
    scale = lax.rsqrt(jnp.mean(values32 * values32, axis=-1, keepdims=True) + EPSILON)
    normed = (values32 * scale * norm_gain).astype(jnp.bfloat16)
    flat_routes = routes.reshape(-1)
    onehot = (flat_routes[:, None] == jnp.arange(targets, dtype=jnp.int32)[None, :]).astype(
        jnp.int32
    )
    earlier_count = jnp.sum((jnp.cumsum(onehot, axis=0) - onehot) * onehot, axis=1)
    slot_index = flat_routes * capacity + earlier_count
    copies = jnp.repeat(normed, choice_count, axis=0)
    outgoing = jnp.zeros((targets * capacity, model_width), jnp.bfloat16).at[slot_index].set(copies)
    outgoing = outgoing.reshape(targets, capacity, model_width)
    arrived = lax.all_to_all(outgoing, "ep", split_axis=0, concat_axis=0, tiled=True)
    flat_rows = arrived.reshape(-1, model_width)
    gate_pre = jnp.dot(flat_rows, gate_weight[0], preferred_element_type=jnp.float32)
    up_pre = jnp.dot(flat_rows, up_weight[0], preferred_element_type=jnp.float32)
    act = clamped_unit(gate_pre, up_pre).astype(jnp.bfloat16)
    result = jnp.dot(act, down_weight[0], preferred_element_type=jnp.float32).astype(jnp.bfloat16)
    came_back = lax.all_to_all(
        result.reshape(arrived.shape), "ep", split_axis=0, concat_axis=0, tiled=True
    )
    picked = came_back.reshape(targets * capacity, model_width)[slot_index]
    weighted = (
        picked.astype(jnp.float32).reshape(tok_rows, choice_count, model_width)
        * route_weight[:, :, None]
    )
    return jnp.sum(weighted, axis=1).astype(jnp.bfloat16)


def ring_order(count):
    return list(range(0, count, 2)) + list(range(count - 1, 0, -2))


def ring_pairs(count, step):
    order = ring_order(count)
    return [(order[at], order[(at + step) % count]) for at in range(count)]


def onward(value):
    return lax.ppermute(value, "ep", ring_pairs(lax.axis_size("ep"), 1))


def backward(value):
    return lax.ppermute(value, "ep", ring_pairs(lax.axis_size("ep"), -1))


def sent_shares(routes, route_weight):
    targets = lax.axis_size("ep")
    names = jnp.arange(targets, dtype=jnp.int32)
    chosen = routes.T[None, :, :] == names[:, None, None]
    shares = jnp.sum(jnp.where(chosen, route_weight.T[None, :, :], 0.0), axis=1)
    return lax.all_to_all(shares, "ep", split_axis=0, concat_axis=0, tiled=True)


def ring_weights(arrived):
    targets = lax.axis_size("ep")
    names = jnp.arange(targets, dtype=jnp.int32)
    order = ring_order(targets)
    places = jnp.asarray([order.index(at) for at in range(targets)], dtype=jnp.int32)
    own = jnp.sum(jnp.where(names == lax.axis_index("ep"), places, 0))
    steps = (places - own) % targets
    picked = names[:, None] == steps[None, :]
    return jnp.sum(jnp.where(picked[:, :, None], arrived[None, :, :], 0.0), axis=1).T


def ring_experts(moe_input, norm_gain, routes, route_weight, gate_weight, up_weight, down_weight):
    tok_rows, _ = moe_input.shape
    targets = lax.axis_size("ep")
    half = targets // 2
    cut = tok_rows // 2
    arrived = sent_shares(routes, route_weight)

    def expert(rows):
        values32 = rows.astype(jnp.float32)
        scale = lax.rsqrt(jnp.mean(values32 * values32, axis=-1, keepdims=True) + EPSILON)
        normed = (values32 * scale * norm_gain).astype(jnp.bfloat16)
        gate_pre = jnp.dot(normed, gate_weight[0], preferred_element_type=jnp.float32)
        up_pre = jnp.dot(normed, up_weight[0], preferred_element_type=jnp.float32)
        act = clamped_unit(gate_pre, up_pre).astype(jnp.bfloat16)
        result = jnp.dot(act, down_weight[0], preferred_element_type=jnp.float32)
        return result.astype(jnp.bfloat16)

    def share(result, step, start, stop):
        weight = block_weights[start:stop, step % targets][:, None]
        return result.astype(jnp.float32) * weight

    results = {}
    ahead = behind = moe_input
    for step in range(1, half):
        ahead, behind = onward(ahead), backward(behind)
        if step == 1:
            results[0] = expert(moe_input)
        both = expert(jnp.concatenate([ahead, behind], axis=0))
        results[-step], results[step] = both[:tok_rows], both[tok_rows:]
        if step == 2:
            block_weights = ring_weights(lax.optimization_barrier((arrived, ahead))[0])
    far_ahead = onward(ahead[:cut])
    far_behind = backward(behind[cut:])
    far = expert(jnp.concatenate([far_ahead, far_behind], axis=0))
    first = onward(share(far[:cut], half, 0, cut).astype(jnp.bfloat16))
    second = backward(share(far[cut:], half, cut, tok_rows).astype(jnp.bfloat16))
    up_own = share(results[half - 1], half - 1, 0, tok_rows)
    down_own = share(results[1 - half], 1 - half, 0, tok_rows)
    up_sum = jnp.concatenate([up_own[:cut] + first.astype(jnp.float32), up_own[cut:]], axis=0)
    down_sum = jnp.concatenate(
        [down_own[:cut], down_own[cut:] + second.astype(jnp.float32)], axis=0
    )
    for step in range(half - 1, 0, -1):
        up_sum = onward(up_sum.astype(jnp.bfloat16)).astype(jnp.float32)
        down_sum = backward(down_sum.astype(jnp.bfloat16)).astype(jnp.float32)
        if step > 1:
            up_sum = up_sum + share(results[step - 1], step - 1, 0, tok_rows)
            down_sum = down_sum + share(results[1 - step], 1 - step, 0, tok_rows)
    own = share(results[0], 0, 0, tok_rows)
    return (own + up_sum + down_sum).astype(jnp.bfloat16)


def by_ring(targets, choice_count):
    return targets % 2 == 0 and 8 <= targets <= 4 * choice_count


def on_device(
    queries,
    head_keys,
    head_values,
    sink_logits,
    out_weight,
    moe_input,
    norm_gain,
    routes,
    route_weight,
    gate_weight,
    up_weight,
    down_weight,
):
    attention_out = attend(queries, head_keys, head_values, sink_logits, out_weight)
    dense = by_ring(lax.axis_size("ep"), routes.shape[1])
    routed_out = (ring_experts if dense else experts_part)(
        moe_input, norm_gain, routes, route_weight, gate_weight, up_weight, down_weight
    )
    return (attention_out, routed_out)


def solution(mesh):
    placed = (
        P("ep", "tp"),
        P("ep", "tp"),
        P("ep", "tp"),
        P("tp"),
        P("tp", None),
        P(("ep", "tp"), None),
        P(),
        P(("ep", "tp"), None),
        P(("ep", "tp"), None),
        P("ep", None, None),
        P("ep", None, None),
        P("ep", None, None),
    )

    return jax.shard_map(
        on_device,
        mesh=mesh,
        in_specs=placed,
        out_specs=(P(("ep", "tp"), None), P(("ep", "tp"), None)),
        check_vma=False,
    )
```
